32 devices in a mesh: kv: 8 (over z, y), tp: 4 (over x, core).
Axes of the slice: x: 2, y: 2, z: 4, core: 2. Of those that a mesh axis runs over, the one named last changes fastest.
Arguments:
- tokens: bfloat16 [4, 4096], P(None, ('kv', 'tp')), may hold values from -6 to 6
- gain_first: bfloat16 [4096], P(('kv', 'tp')), may hold values from 0.099609375 to 1.8984375
- w_query: bfloat16 [4096, 2048], P('kv', 'tp'), may hold values from -0.09375 to 0.09375
- w_key: bfloat16 [4096, 2048], P('kv', 'tp'), may hold values from -0.09375 to 0.09375
- w_value: bfloat16 [4096, 2048], P('kv', 'tp'), may hold values from -0.09375 to 0.09375
- w_forget: bfloat16 [4096, 32], P('kv'), may hold values from -0.1875 to 0.1875
- forget_bias: float32 [32], P('tp'), may hold values from 1 to 6
- past_keys: bfloat16 [4, 16384, 2048], P(None, 'kv', 'tp'), may hold values from -48 to 48
- past_values: bfloat16 [4, 16384, 2048], P(None, 'kv', 'tp'), may hold values from -6 to 6
- past_forget: float32 [4, 32, 16384], P(None, 'tp', 'kv'), may hold values from -0.25 to 0, as said below
- w_out: bfloat16 [2048, 4096], P('tp', 'kv'), may hold values from -0.5 to 0.5
- gain_second: bfloat16 [4096], P(('kv', 'tp')), may hold values from 0.099609375 to 1.8984375
- w_gate: bfloat16 [4096, 11264], P(None, ('kv', 'tp')), may hold values from -0.09375 to 0.09375
- w_up: bfloat16 [4096, 11264], P(None, ('kv', 'tp')), may hold values from -0.09375 to 0.09375
- w_down: bfloat16 [11264, 4096], P(('kv', 'tp')), may hold values from -0.109375 to 0.109375
Outputs:
- layer_out: bfloat16 [4, 4096], P(None, ('kv', 'tp'))
- new_keys: bfloat16 [4, 2048], P(None, 'tp')
- new_values: bfloat16 [4, 2048], P(None, 'tp')
- new_forget: float32 [4, 32], P(None, 'tp')
The draws below stay inside these ranges and needn't reach their ends.
Inputs may be any that keep to these rules, and one draw needn't show every extreme that they name: `past_forget`: each entry is the logarithm of a forget gate: negative, and no smaller than -0.25.
All inputs are finite; a program needn't handle non-finite values.
Results may differ from the reference program's by a relative error of at most 0.0095.
The reference program's roundings to bfloat16 on the way count: a program that leaves them out, or rounds other values in their place, can miss the bound.
Values may be sent and summed in bfloat16 or wider, within the bound.
A program may use at most 128 MiB of HBM per device.

```python
import jax
import jax.numpy as jnp
from jax import lax

D = 4096
HEADS = 32
FF = 11264
BATCH = 4
CACHE_DEV = 2048
D_ATTN = 2048
CACHE = 16384
N_KV = 8


def draw_past_keys(key, part):
    normal_key = jax.random.fold_in(key, 0)
    drawn = jnp.clip(jax.random.normal(normal_key, (BATCH, CACHE, D_ATTN), jnp.float32), -6.0, 6.0)
    return drawn.astype(jnp.bfloat16)


def draw_past_forget(key, part):
    level_key, keep_key, phase_key, noise_key = jax.random.split(key, 4)
    head_index = jnp.arange(HEADS)
    short_level = jnp.log(jax.random.uniform(level_key, (HEADS,), jnp.float32, 30.0, 200.0))
    long_level = jnp.log(CACHE / jax.random.uniform(keep_key, (HEADS,), jnp.float32, 0.1, 3.0))
    levels = jnp.where(head_index % 2 == 0, short_level, long_level)
    positions = jnp.arange(CACHE).astype(jnp.float32) / CACHE
    phases = jax.random.uniform(phase_key, (BATCH, HEADS, 1), jnp.float32, 0.0, 6.283185307)
    drift_wave = 0.7 * jnp.sin(6.283185307 * 3.0 * positions[None, None, :] + phases)
    jitter = jnp.clip(0.3 * jax.random.normal(noise_key, (BATCH, HEADS, CACHE), jnp.float32), -0.9, 0.9)
    preact = levels[None, :, None] + drift_wave + jitter
    return jax.nn.log_sigmoid(preact).astype(jnp.float32)


def strengthened(entries, rng, source, target, parts, factor):
    owner, partner = [(jnp.arange(entries.shape[dim]) // (entries.shape[dim] // parts)).reshape([-1 if axis == dim else 1 for axis in range(entries.ndim)]) for dim in (source, target)]
    chosen = jax.random.permutation(rng, parts)[partner]
    strong = (owner == chosen) | (owner == (partner + parts // 2) % parts)
    return jnp.where(strong, factor * entries, entries)


def shard_levels(own_key, extent, shards, least, high):
    gain, own = 1.0, jax.random.fold_in(own_key, 6)
    for dim, parts in shards:
        heights = jnp.exp(jax.random.uniform(jax.random.fold_in(own, dim), (parts,), jnp.float32, least / len(shards), high / len(shards)))
        gain = gain * jnp.repeat(heights, extent[dim] // parts).reshape([-1 if axis == dim else 1 for axis in range(len(extent))])
    return gain


def bell_draw(own_key, shape, scale, most, pieces=(), kind=jnp.bfloat16):
    array = scale * jax.random.normal(own_key, shape, jnp.float32)
    if pieces:
        array = array * shard_levels(own_key, shape, pieces, -0.22, 0.18)
    return jnp.clip(array, -most, most).astype(kind)


def heavy_noise(key, dims, scale, most, cuts, heavy, kind=jnp.bfloat16):
    values = scale * jax.random.normal(key, dims, jnp.float32)
    if cuts:
        values = values * shard_levels(key, dims, cuts, -0.22, 0.18)
    return jnp.clip(strengthened(values, jax.random.fold_in(key, 3), *heavy), -most, most).astype(kind)


def setup_inputs(seed: int = 0) -> dict:
    key_list = jax.random.split(jax.random.key(seed), 16)
    tokens = bell_draw(key_list[0], (BATCH, D), 1.0, 6.0, ((1, 32),))
    gain_first = jnp.clip(1.0 + 0.18 * jax.random.normal(key_list[1], (D,), jnp.float32), 0.099609375, 1.8984375).astype(jnp.bfloat16)
    w_query = bell_draw(key_list[2], (D, D_ATTN), D ** -0.5, 0.09375, ((0, 8), (1, 4)))
    w_key = bell_draw(key_list[3], (D, D_ATTN), D ** -0.5, 0.09375, ((0, 8), (1, 4)))
    w_value = bell_draw(key_list[4], (D, D_ATTN), D ** -0.5, 0.09375, ((0, 8), (1, 4)))
    w_forget = bell_draw(key_list[5], (D, HEADS), (D // 4) ** -0.5, 0.1875, ((0, 8),))
    forget_bias = jnp.clip(1.0 + 5.0 * jax.random.uniform(key_list[6], (HEADS,), jnp.float32) ** shard_levels(key_list[6], (HEADS,), ((0, 4),), -0.2, 0.2), 1.0, 6.0)
    past_keys = draw_past_keys(jax.random.fold_in(key_list[15], 71), 0)
    past_values = bell_draw(key_list[8], (BATCH, CACHE, D_ATTN), 1.0, 6.0, ((1, 8), (2, 4)))
    past_forget = draw_past_forget(jax.random.fold_in(key_list[15], 71), 0)
    w_out = bell_draw(key_list[10], (D_ATTN, D), (D_ATTN // 16) ** -0.5, 0.5, ((0, 4), (1, 8)))
    gain_second = jnp.clip(1.0 + 0.18 * jax.random.normal(key_list[11], (D,), jnp.float32), 0.099609375, 1.8984375).astype(jnp.bfloat16)
    w_gate = bell_draw(key_list[12], (D, FF), D ** -0.5, 0.09375, ((1, 32),))
    w_up = bell_draw(key_list[13], (D, FF), D ** -0.5, 0.09375, ((1, 32),))
    w_down = heavy_noise(key_list[14], (FF, D), FF ** -0.5, 0.109375, ((0, 32),), (0, 1, 32, 2.75))
    return dict(tokens=tokens, gain_first=gain_first, w_query=w_query, w_key=w_key, w_value=w_value, w_forget=w_forget, forget_bias=forget_bias, past_keys=past_keys, past_values=past_values, past_forget=past_forget, w_out=w_out, gain_second=gain_second, w_gate=w_gate, w_up=w_up, w_down=w_down)


epsilon = 1e-05
highest_precision = lax.Precision.HIGHEST

def row_scales(first_sum, second_sum, row_width):
    row_mean = first_sum / row_width
    spread = jnp.maximum(second_sum / row_width - row_mean * row_mean, 0.0) + epsilon
    return (row_mean, lax.rsqrt(spread))

def reference(tokens, gain_first, w_query, w_key, w_value, w_forget, forget_bias, past_keys, past_values, past_forget, w_out, gain_second, w_gate, w_up, w_down):
    wide_rows = tokens.astype(jnp.float32)
    row_width = tokens.shape[1]
    row_mean, row_scale = row_scales(lax.optimization_barrier(jnp.sum(wide_rows, axis=1, keepdims=True)), lax.optimization_barrier(jnp.sum(wide_rows * wide_rows, axis=1, keepdims=True)), row_width)
    scaled = (wide_rows * gain_first.astype(jnp.float32)).astype(jnp.bfloat16)

    def project(weight):
        product = jnp.dot(scaled, weight, preferred_element_type=jnp.float32)
        column = jnp.dot(gain_first[None, :], weight, preferred_element_type=jnp.float32)
        return row_scale * (product - row_mean * column)
    query = project(w_query).astype(jnp.bfloat16)
    new_keys = project(w_key).astype(jnp.bfloat16)
    new_values = project(w_value).astype(jnp.bfloat16)
    new_forget = jax.nn.log_sigmoid(project(w_forget) + forget_bias)
    batch_rows = tokens.shape[0]
    heads_all = forget_bias.shape[0]
    head_size = query.shape[1] // heads_all
    score_scale = head_size ** (-0.5)
    span_block = CACHE_DEV
    suffix = jnp.cumsum(past_forget[:, :, ::-1], axis=2)[:, :, ::-1] - past_forget
    decay_bias = new_forget[:, :, None] + suffix
    query_heads = lax.optimization_barrier(query).astype(jnp.float32).reshape(batch_rows, heads_all, head_size)

    def block_terms(offset):
        key_block = lax.dynamic_slice_in_dim(past_keys, offset, span_block, 1).astype(jnp.float32).reshape(batch_rows, span_block, heads_all, head_size)
        value_block = lax.dynamic_slice_in_dim(past_values, offset, span_block, 1).astype(jnp.float32).reshape(batch_rows, span_block, heads_all, head_size)
        bias_block = lax.dynamic_slice_in_dim(decay_bias, offset, span_block, 2)
        logits = jnp.einsum('bhd,bshd->bhs', query_heads, key_block, precision=highest_precision) * score_scale + bias_block
        block_top = lax.optimization_barrier(jnp.max(logits, axis=2))
        weights = jnp.exp(logits - block_top[:, :, None])
        block_sum = lax.optimization_barrier(jnp.sum(weights, axis=2))
        rounded = lax.optimization_barrier(weights.astype(jnp.bfloat16)).astype(jnp.float32)
        block_mix = jnp.einsum('bhs,bshd->bhd', rounded, value_block, precision=highest_precision).astype(jnp.bfloat16)
        return (block_top, block_sum, lax.optimization_barrier(block_mix).astype(jnp.float32))
    offsets = jnp.arange(N_KV, dtype=jnp.int32) * span_block
    all_tops, all_sums, all_mixes = lax.map(block_terms, offsets)
    highest = lax.optimization_barrier(jnp.max(all_tops, axis=0))
    factors = jnp.exp(all_tops - highest[None])
    totals = lax.optimization_barrier(jnp.sum(all_sums * factors, axis=0))
    mixtures = lax.optimization_barrier(jnp.sum(all_mixes * factors[..., None], axis=0))
    own_keys = lax.optimization_barrier(new_keys).astype(jnp.float32).reshape(batch_rows, heads_all, head_size)
    own_values = lax.optimization_barrier(new_values).astype(jnp.float32).reshape(batch_rows, heads_all, head_size)
    own_score = jnp.einsum('bhd,bhd->bh', query_heads, own_keys, precision=highest_precision) * score_scale
    top_all = jnp.maximum(highest, own_score)
    old_factor = jnp.exp(highest - top_all)
    new_factor = jnp.exp(own_score - top_all)
    attended = (mixtures * old_factor[..., None] + own_values * new_factor[..., None]) / (totals * old_factor + new_factor)[..., None]
    attended = attended.reshape(batch_rows, heads_all * head_size).astype(jnp.bfloat16)
    branch = jnp.dot(attended, w_out, preferred_element_type=jnp.float32)
    middle = (wide_rows + branch).astype(jnp.bfloat16)
    wide_mid = lax.optimization_barrier(middle).astype(jnp.float32)
    mid_mean, mid_scale = row_scales(lax.optimization_barrier(jnp.sum(wide_mid, axis=1, keepdims=True)), lax.optimization_barrier(jnp.sum(wide_mid * wide_mid, axis=1, keepdims=True)), row_width)
    normed = ((wide_mid - mid_mean) * mid_scale * gain_second.astype(jnp.float32)).astype(jnp.bfloat16)
    gate_acc = jnp.dot(normed, w_gate, preferred_element_type=jnp.float32)
    up_acc = jnp.dot(normed, w_up, preferred_element_type=jnp.float32)
    hidden = (jax.nn.silu(gate_acc) * up_acc).astype(jnp.bfloat16)
    channel = jnp.dot(hidden, w_down, preferred_element_type=jnp.float32)
    layer_out = (wide_mid + channel).astype(jnp.bfloat16)
    return (layer_out, new_keys, new_values, new_forget)
```

```python
import functools

import jax
import jax.numpy as jnp
from jax import lax
from jax.experimental import pallas as pl
from jax.experimental.pallas import tpu as pltpu
from jax.sharding import PartitionSpec as P

epsilon = 1e-05
MESH = pl.DeviceIdType.MESH
HIGHEST = lax.Precision.HIGHEST
LANES = 128
F32 = jnp.float32
BF16 = jnp.bfloat16


def iota(shape, dim):
    return lax.broadcasted_iota(jnp.int32, shape, dim)


def row_scales(first_sum, second_sum, row_width):
    row_mean = first_sum / row_width
    spread = jnp.maximum(second_sum / row_width - row_mean * row_mean, 0.0) + epsilon
    return (row_mean, lax.rsqrt(spread))


def kernel(
    nkv,
    ntp,
    tokens_h,
    gain1_h,
    wq_h,
    wk_h,
    wv_h,
    wf_h,
    fb_h,
    pk_h,
    pv_h,
    pf_h,
    wo_h,
    gain2_h,
    wg_h,
    wu_h,
    wd_h,
    out_ref,
    nk_ref,
    nv_ref,
    nf_ref,
    tokens_v,
    gain1_v,
    gain2_v,
    wq_v,
    wk_v,
    wv_v,
    wf_v,
    fb_v,
    pk_v,
    pv_v,
    pf_v,
    wo_v,
    wg_v,
    wu_v,
    wd_v,
    gat,
    xbuf,
    qmsg,
    kvmsg,
    sfx,
    mixbuf,
    amix,
    astat,
    coef,
    bmsg,
    mpieces,
    mmsg,
    mbuf,
    gbuf,
    fsend,
    frecv,
    in_sem,
    s1,
    r1,
    sq,
    rq,
    sk,
    rk,
    sa,
    ra,
    st,
    rt,
    sb,
    rb,
    sm,
    rm,
    sf,
    rf,
):
    i = lax.axis_index("kv")
    j = lax.axis_index("tp")
    B, c0 = tokens_v.shape
    R, C = wq_v.shape
    H = wf_v.shape[1]
    h = fb_v.shape[1]
    hd = C // h
    S = pk_v.shape[1]
    D, F = wg_v.shape
    N = nkv * ntp
    scale = hd ** (-0.5)
    nc, nr = C // LANES, R // LANES

    plan = [
        (tokens_h, tokens_v),
        (gain1_h, gain1_v),
        (gain2_h, gain2_v),
        (wq_h, wq_v),
        (wf_h, wf_v),
        (wk_h, wk_v),
        (wv_h, wv_v),
        (pf_h, pf_v),
    ]
    plan += [(pk_h.at[b], pk_v.at[b]) for b in range(B)]
    plan += [(pv_h.at[b], pv_v.at[b]) for b in range(B)]
    plan += [(fb_h, fb_v), (wo_h, wo_v), (wg_h, wg_v), (wu_h, wu_v), (wd_h, wd_v)]
    loads = [
        pltpu.make_async_copy(src, dst, in_sem.at[n]) for n, (src, dst) in enumerate(plan)
    ]
    for load in loads:
        load.start()
    l_tok, l_g1, l_g2, l_wq, l_wf, l_wk, l_wv, l_pf = loads[:8]
    l_pk, l_pv = loads[8 : 8 + B], loads[8 + B : 8 + 2 * B]
    l_fb, l_wo, l_wg, l_wu, l_wd = loads[8 + 2 * B :]

    barrier = pltpu.get_barrier_semaphore()
    for a in range(nkv):
        for b in range(ntp):
            if a or b:
                pl.semaphore_signal(
                    barrier,
                    inc=1,
                    device_id=(lax.rem(i + a, nkv), lax.rem(j + b, ntp)),
                    device_id_type=MESH,
                )

    pending = []

    def to_kv(buf, ssem, rsem):
        for o in range(1, nkv):
            copy = pltpu.make_async_remote_copy(
                src_ref=buf.at[i],
                dst_ref=buf.at[i],
                send_sem=ssem.at[o],
                recv_sem=rsem.at[o],
                device_id=(lax.rem(i + o, nkv), j),
                device_id_type=MESH,
            )
            copy.start()
            pending.append(copy)

    def from_kv(buf, ssem, rsem):
        for o in range(1, nkv):
            slot = lax.rem(i + nkv - o, nkv)
            pltpu.make_async_remote_copy(
                src_ref=buf.at[slot],
                dst_ref=buf.at[slot],
                send_sem=ssem.at[o],
                recv_sem=rsem.at[o],
                device_id=(slot, j),
                device_id_type=MESH,
            ).wait_recv()

    def to_tp(buf, ssem, rsem):
        for o in range(1, ntp):
            copy = pltpu.make_async_remote_copy(
                src_ref=buf.at[j],
                dst_ref=buf.at[j],
                send_sem=ssem.at[o],
                recv_sem=rsem.at[o],
                device_id=(i, lax.rem(j + o, ntp)),
                device_id_type=MESH,
            )
            copy.start()
            pending.append(copy)

    def from_tp(buf, ssem, rsem):
        for o in range(1, ntp):
            slot = lax.rem(j + ntp - o, ntp)
            pltpu.make_async_remote_copy(
                src_ref=buf.at[slot],
                dst_ref=buf.at[slot],
                send_sem=ssem.at[o],
                recv_sem=rsem.at[o],
                device_id=(i, slot),
                device_id_type=MESH,
            ).wait_recv()

    l_tok.wait()
    l_g1.wait()
    l_g2.wait()
    gat[j, 0:B, :] = tokens_v[...].astype(F32)
    gat[j, B : B + 1, :] = gain1_v[...].astype(F32)
    gat[j, B + 1 : B + 2, :] = gain2_v[...].astype(F32)
    gat[j, B + 2 : 8, :] = jnp.zeros((6 - B, c0), F32)
    pl.semaphore_wait(barrier, N - 1)
    to_tp(gat, s1, r1)
    l_wq.wait()
    l_wf.wait()
    from_tp(gat, s1, r1)
    for t in range(ntp):
        xbuf[:, t * c0 : (t + 1) * c0] = gat[t]

    every = xbuf[...]
    rows = every[0:B]
    gain_b = jnp.broadcast_to(every[B : B + 1], every.shape)
    row_id = iota(every.shape, 0)
    lhs = jnp.where(row_id < B, every * gain_b, jnp.where(row_id == B, gain_b, 0.0)).astype(BF16)

    def product(weight):
        return jnp.dot(lhs, weight[...], preferred_element_type=F32)

    def spread(buf, at, row, count):
        if count < B:
            buf[i, :, at : at + LANES] = jnp.zeros((B, LANES), F32)
        for r in range(count):
            buf[i, r : r + 1, at : at + LANES] = row[:, r * LANES : (r + 1) * LANES]

    part = product(wq_v)
    qmsg[i, :, 0:C] = part[0:B]
    spread(qmsg, C, part[B : B + 1], nc)
    part = product(wf_v)
    aux = C + LANES
    qmsg[i, :, aux : aux + LANES] = jnp.zeros((B, LANES), F32)
    qmsg[i, :, aux : aux + H] = part[0:B]
    qmsg[i, :, aux + H : aux + 2 * H] = jnp.broadcast_to(part[B : B + 1], (B, H))
    qmsg[i, :, aux + 2 * H : aux + 2 * H + 1] = jnp.sum(rows, axis=1, keepdims=True)
    qmsg[i, :, aux + 2 * H + 1 : aux + 2 * H + 2] = jnp.sum(rows * rows, axis=1, keepdims=True)
    to_kv(qmsg, sq, rq)

    l_wk.wait()
    part = product(wk_v)
    kvmsg[i, :, 0:C] = part[0:B]
    spread(kvmsg, 2 * C, part[B : B + 1], nc)
    l_wv.wait()
    part = product(wv_v)
    kvmsg[i, :, C : 2 * C] = part[0:B]
    spread(kvmsg, 2 * C + LANES, part[B : B + 1], nc)
    spread(kvmsg, 2 * C + 2 * LANES, every[B + 1 : B + 2], nr)
    to_kv(kvmsg, sk, rk)

    l_pf.wait()
    later = (iota((LANES, LANES), 0) > iota((LANES, LANES), 1)).astype(F32)
    carry = jnp.zeros((B * h, 1), F32)
    for c in reversed(range(S // LANES)):
        cols = slice(c * LANES, (c + 1) * LANES)
        chunk = jnp.concatenate([pf_v[b, :, cols] for b in range(B)], axis=0)
        inside = jnp.dot(chunk, later, precision=HIGHEST, preferred_element_type=F32)
        whole = inside + carry
        for b in range(B):
            sfx[b, :, cols] = whole[b * h : (b + 1) * h]
        carry = carry + (inside[:, 0:1] + chunk[:, 0:1])

    from_kv(qmsg, sq, rq)
    total = qmsg[0]
    for n in range(1, nkv):
        total = total + qmsg[n]
    moments = total[:, aux + 2 * H : aux + 2 * H + 2]
    mean, factor = row_scales(moments[:, 0:1], moments[:, 1:2], D)

    def whole_row(array, at, count):
        return jnp.concatenate([array[r : r + 1, at : at + LANES] for r in range(count)], axis=1)

    def finish(product_, gain_row):
        return factor * (product_ - mean * gain_row)

    query = finish(total[:, 0:C], whole_row(total, C, nc)).astype(BF16).astype(F32)

    head_of = iota((h, C), 1) // hd
    mine = head_of == iota((h, C), 0)
    head_row = iota((h, LANES), 0)
    lane = iota((h, LANES), 1)
    for b in range(B):
        spread_q = jnp.where(mine, jnp.broadcast_to(query[b : b + 1], (h, C)), 0.0).astype(BF16)
        l_pk[b].wait()
        scores = lax.dot_general(
            spread_q, pk_v[b], (((1,), (1,)), ((), ())), preferred_element_type=F32
        )
        logits = scores * scale + sfx[b]
        top = jnp.max(logits, axis=1, keepdims=True)
        weights = jnp.exp(logits - top)
        amount = jnp.sum(weights, axis=1, keepdims=True)
        l_pv[b].wait()
        mixed = jnp.dot(weights.astype(BF16), pv_v[b], preferred_element_type=F32)
        mixbuf[b : b + 1, :] = jnp.sum(jnp.where(mine, mixed, 0.0), axis=0, keepdims=True)
        marks = (
            jnp.where(lane == head_row, top, 0.0)
            + jnp.where(lane == head_row + 32, amount, 0.0)
            + jnp.where(lane == head_row + 64, carry[b * h : (b + 1) * h], 0.0)
        )
        astat[i, b : b + 1, :] = jnp.sum(marks, axis=0, keepdims=True)
    amix[i] = mixbuf[...].astype(BF16)
    to_kv(astat, st, rt)
    to_kv(amix, sa, ra)

    from_kv(kvmsg, sk, rk)
    pair = kvmsg[0, :, 0 : 2 * C + 2 * LANES]
    for n in range(1, nkv):
        pair = pair + kvmsg[n, :, 0 : 2 * C + 2 * LANES]
    for n in range(nkv):
        for r in range(nr):
            at = n * R + r * LANES
            gbuf[0:1, at : at + LANES] = kvmsg[n, r : r + 1, 2 * C + 2 * LANES : 2 * C + 3 * LANES]
    new_keys = finish(pair[:, 0:C], whole_row(pair, 2 * C, nc)).astype(BF16)
    new_values = finish(pair[:, C : 2 * C], whole_row(pair, 2 * C + LANES, nc)).astype(BF16)
    nk_ref[...] = new_keys
    nv_ref[...] = new_values
    pre = finish(total[:, aux : aux + H], total[:, aux + H : aux + 2 * H])
    pick = (iota((H, LANES), 0) == iota((H, LANES), 1) + j * h).astype(F32)
    l_fb.wait()
    gates = jnp.dot(pre, pick, precision=HIGHEST, preferred_element_type=F32)[:, 0:h] + fb_v[...]
    new_forget = jnp.minimum(gates, 0.0) - jnp.log1p(jnp.exp(-jnp.abs(gates)))
    nf_ref[...] = new_forget
    expand = (iota((LANES, C), 0) == iota((LANES, C), 1) // hd).astype(F32)
    gather = (iota((C, LANES), 0) // hd == iota((C, LANES), 1)).astype(F32)
    own = (
        jnp.dot(
            query * new_keys.astype(F32), gather, precision=HIGHEST, preferred_element_type=F32
        )[:, 0:h]
        * scale
    )
    coef[...] = jnp.zeros(coef.shape, F32)
    l_wo.wait()

    from_kv(astat, st, rt)
    tops, amounts = [None] * nkv, [None] * nkv
    behind = new_forget
    peak = own
    for n in reversed(range(nkv)):
        tops[n] = astat[n, :, 0:h] + behind
        amounts[n] = astat[n, :, 32 : 32 + h]
        behind = behind + astat[n, :, 64 : 64 + h]
        peak = jnp.maximum(peak, tops[n])
    own_part = jnp.exp(own - peak)
    bottom = own_part
    parts = []
    for n in range(nkv):
        parts.append(jnp.exp(tops[n] - peak))
        bottom = bottom + amounts[n] * parts[n]
    for n, one in enumerate(parts + [own_part]):
        coef[n * B : (n + 1) * B, 0:h] = one / bottom
    wide = jnp.dot(coef[...], expand, precision=HIGHEST, preferred_element_type=F32)
    attended = wide[nkv * B : (nkv + 1) * B] * new_values.astype(F32)
    from_kv(amix, sa, ra)
    for n in range(nkv):
        attended = attended + wide[n * B : (n + 1) * B] * amix[n].astype(F32)

    bmsg[j] = jnp.dot(attended.astype(BF16), wo_v[...], preferred_element_type=F32)
    to_tp(bmsg, sb, rb)
    from_tp(bmsg, sb, rb)
    branch = bmsg[0]
    for t in range(1, ntp):
        branch = branch + bmsg[t]
    middle = (rows + branch).astype(BF16)
    mmsg[i] = middle
    to_kv(mmsg, sm, rm)
    for t in range(ntp):
        mpieces[t] = middle[:, t * c0 : (t + 1) * c0].astype(F32)
    l_wg.wait()
    l_wu.wait()
    l_wd.wait()
    from_kv(mmsg, sm, rm)
    for n in range(nkv):
        mbuf[:, n * R : (n + 1) * R] = mmsg[n].astype(F32)
    wide_mid = mbuf[...]
    mid_mean, mid_scale = row_scales(
        jnp.sum(wide_mid, axis=1, keepdims=True),
        jnp.sum(wide_mid * wide_mid, axis=1, keepdims=True),
        D,
    )
    normed = ((wide_mid - mid_mean) * mid_scale * gbuf[...]).astype(BF16)
    gate = jnp.dot(normed, wg_v[...], preferred_element_type=F32)
    up = jnp.dot(normed, wu_v[...], preferred_element_type=F32)
    hidden = (gate / (1.0 + jnp.exp(-gate)) * up).astype(BF16)
    down = jnp.dot(hidden, wd_v[...], preferred_element_type=F32)
    for p in range(N):
        fsend[p] = down[:, p * c0 : (p + 1) * c0]
    me = i * ntp + j
    for a in reversed(range(nkv)):
        for b in range(ntp):
            if a or b:
                there = (lax.rem(i + a, nkv), lax.rem(j + b, ntp))
                copy = pltpu.make_async_remote_copy(
                    src_ref=fsend.at[there[0] * ntp + there[1]],
                    dst_ref=frecv.at[me],
                    send_sem=sf.at[a * ntp + b],
                    recv_sem=rf.at[a * ntp + b],
                    device_id=there,
                    device_id_type=MESH,
                )
                copy.start()
                pending.append(copy)
    frecv[me] = fsend[me]
    for a in range(nkv):
        for b in range(ntp):
            if a or b:
                there = (lax.rem(i + nkv - a, nkv), lax.rem(j + ntp - b, ntp))
                slot = there[0] * ntp + there[1]
                pltpu.make_async_remote_copy(
                    src_ref=fsend.at[slot],
                    dst_ref=frecv.at[slot],
                    send_sem=sf.at[a * ntp + b],
                    recv_sem=rf.at[a * ntp + b],
                    device_id=there,
                    device_id_type=MESH,
                ).wait_recv()
    channel = frecv[0]
    for p in range(1, N):
        channel = channel + frecv[p]
    out_ref[...] = (mpieces[j] + channel).astype(BF16)
    for copy in pending:
        copy.wait_send()


def local(nkv, ntp, *arrays):
    (tokens, gain1, wq, wk, wv, wf, fb, pk, pv, pf, wo, gain2, wg, wu, wd) = arrays
    gain1, gain2, fb = gain1[None, :], gain2[None, :], fb[None, :]
    arrays = (tokens, gain1, wq, wk, wv, wf, fb, pk, pv, pf, wo, gain2, wg, wu, wd)
    B, c0 = tokens.shape
    R, C = wq.shape
    h = fb.shape[1]
    D, F = wg.shape
    S = pk.shape[1]
    N = nkv * ntp
    dma = lambda n: pltpu.SemaphoreType.DMA((n,))
    scratch = [
        pltpu.VMEM(a.shape, a.dtype)
        for a in (tokens, gain1, gain2, wq, wk, wv, wf, fb, pk, pv, pf, wo, wg, wu, wd)
    ]
    scratch += [
        pltpu.VMEM((ntp, 8, c0), F32),
        pltpu.VMEM((8, R), F32),
        pltpu.VMEM((nkv, B, C + 2 * LANES), F32),
        pltpu.VMEM((nkv, B, 2 * C + 3 * LANES), F32),
        pltpu.VMEM((B, h, S), F32),
        pltpu.VMEM((B, C), F32),
        pltpu.VMEM((nkv, B, C), BF16),
        pltpu.VMEM((nkv, B, LANES), F32),
        pltpu.VMEM(((nkv + 1) * B, LANES), F32),
        pltpu.VMEM((ntp, B, R), F32),
        pltpu.VMEM((ntp, B, c0), F32),
        pltpu.VMEM((nkv, B, R), BF16),
        pltpu.VMEM((B, D), F32),
        pltpu.VMEM((1, D), F32),
        pltpu.VMEM((N, B, c0), F32),
        pltpu.VMEM((N, B, c0), F32),
        dma(13 + 2 * B),
    ]
    for n in (ntp, nkv, nkv, nkv, nkv, ntp, nkv, N):
        scratch += [dma(n), dma(n)]
    vmem = pl.BlockSpec(memory_space=pltpu.VMEM)
    return pl.pallas_call(
        functools.partial(kernel, nkv, ntp),
        out_shape=(
            jax.ShapeDtypeStruct((B, c0), BF16),
            jax.ShapeDtypeStruct((B, C), BF16),
            jax.ShapeDtypeStruct((B, C), BF16),
            jax.ShapeDtypeStruct((B, h), F32),
        ),
        in_specs=[pl.BlockSpec(memory_space=pl.ANY)] * len(arrays),
        out_specs=(vmem,) * 4,
        scratch_shapes=scratch,
        compiler_params=pltpu.CompilerParams(
            collective_id=0, has_side_effects=True, vmem_limit_bytes=60 * 2**20
        ),
    )(*arrays)


def solution(mesh):
    in_specs = (
        P(None, ("kv", "tp")),
        P(("kv", "tp")),
        P("kv", "tp"),
        P("kv", "tp"),
        P("kv", "tp"),
        P("kv", None),
        P("tp"),
        P(None, "kv", "tp"),
        P(None, "kv", "tp"),
        P(None, "tp", "kv"),
        P("tp", "kv"),
        P(("kv", "tp")),
        P(None, ("kv", "tp")),
        P(None, ("kv", "tp")),
        P(("kv", "tp"), None),
    )
    out_specs = (P(None, ("kv", "tp")), P(None, "tp"), P(None, "tp"), P(None, "tp"))
    step = functools.partial(local, mesh.shape["kv"], mesh.shape["tp"])
    return jax.shard_map(step, mesh=mesh, in_specs=in_specs, out_specs=out_specs, check_vma=False)
```

```python
import functools

import jax
import jax.numpy as jnp
from jax import lax
from jax.experimental import pallas as pl
from jax.experimental.pallas import tpu as pltpu
from jax.sharding import PartitionSpec as P

epsilon = 1e-05
MESH = pl.DeviceIdType.MESH
HIGHEST = lax.Precision.HIGHEST
LANES = 128
F32 = jnp.float32
BF16 = jnp.bfloat16


def iota(shape, dim):
    return lax.broadcasted_iota(jnp.int32, shape, dim)


def across(left, right):
    return lax.dot_general(left, right, (((1,), (1,)), ((), ())), preferred_element_type=F32)


def row_scales(first_sum, second_sum, row_width):
    row_mean = first_sum / row_width
    spread = jnp.maximum(second_sum / row_width - row_mean * row_mean, 0.0) + epsilon
    return (row_mean, lax.rsqrt(spread))


def kernel(
    nkv,
    ntp,
    tokens_h,
    gain1_h,
    wq_h,
    wk_h,
    wv_h,
    wf_h,
    fb_h,
    pk_h,
    pv_h,
    pf_h,
    wo_h,
    gain2_h,
    wg_h,
    wu_h,
    wd_h,
    out_ref,
    nk_ref,
    nv_ref,
    nf_ref,
    tokens_v,
    gain1_v,
    gain2_v,
    wq_v,
    wk_v,
    wv_v,
    wf_v,
    fb_v,
    pk_v,
    pv_v,
    pf_v,
    wo_v,
    wg_v,
    wu_v,
    wd_v,
    gat,
    xbuf,
    qmsg,
    kvmsg,
    sfx,
    mixbuf,
    amix,
    astat,
    coef,
    bmsg,
    mpieces,
    mmsg,
    mbuf,
    gbuf,
    fsend,
    frecv,
    in_sem,
    s1,
    r1,
    sq,
    rq,
    sk,
    rk,
    sa,
    ra,
    st,
    rt,
    sb,
    rb,
    sm,
    rm,
    sf,
    rf,
):
    i = lax.axis_index("kv")
    j = lax.axis_index("tp")
    B, c0 = tokens_v.shape
    R, C = wq_v.shape
    H = wf_v.shape[0]
    h = fb_v.shape[1]
    hd = C // h
    S = pk_v.shape[1]
    F, D = wg_v.shape
    N = nkv * ntp
    scale = hd ** (-0.5)
    nc, nr = C // LANES, R // LANES

    plan = [
        (tokens_h, tokens_v),
        (gain1_h, gain1_v),
        (gain2_h, gain2_v),
        (wq_h, wq_v),
        (wf_h, wf_v),
        (wk_h, wk_v),
        (wv_h, wv_v),
        (pf_h, pf_v),
    ]
    plan += [(pk_h.at[b], pk_v.at[b]) for b in range(B)]
    plan += [(pv_h.at[b], pv_v.at[b]) for b in range(B)]
    plan += [(fb_h, fb_v), (wo_h, wo_v), (wg_h, wg_v), (wu_h, wu_v), (wd_h, wd_v)]
    loads = [
        pltpu.make_async_copy(src, dst, in_sem.at[n]) for n, (src, dst) in enumerate(plan)
    ]
    for load in loads:
        load.start()
    l_tok, l_g1, l_g2, l_wq, l_wf, l_wk, l_wv, l_pf = loads[:8]
    l_pk, l_pv = loads[8 : 8 + B], loads[8 + B : 8 + 2 * B]
    l_fb, l_wo, l_wg, l_wu, l_wd = loads[8 + 2 * B :]

    barrier = pltpu.get_barrier_semaphore()
    for a in range(nkv):
        for b in range(ntp):
            if a or b:
                pl.semaphore_signal(
                    barrier,
                    inc=1,
                    device_id=(lax.rem(i + a, nkv), lax.rem(j + b, ntp)),
                    device_id_type=MESH,
                )

    pending = []

    def to_kv(buf, ssem, rsem):
        for o in range(1, nkv):
            copy = pltpu.make_async_remote_copy(
                src_ref=buf.at[i],
                dst_ref=buf.at[i],
                send_sem=ssem.at[o],
                recv_sem=rsem.at[o],
                device_id=(lax.rem(i + o, nkv), j),
                device_id_type=MESH,
            )
            copy.start()
            pending.append(copy)

    def from_kv(buf, ssem, rsem):
        for o in range(1, nkv):
            slot = lax.rem(i + nkv - o, nkv)
            pltpu.make_async_remote_copy(
                src_ref=buf.at[slot],
                dst_ref=buf.at[slot],
                send_sem=ssem.at[o],
                recv_sem=rsem.at[o],
                device_id=(slot, j),
                device_id_type=MESH,
            ).wait_recv()

    def to_tp(buf, ssem, rsem):
        for o in range(1, ntp):
            copy = pltpu.make_async_remote_copy(
                src_ref=buf.at[j],
                dst_ref=buf.at[j],
                send_sem=ssem.at[o],
                recv_sem=rsem.at[o],
                device_id=(i, lax.rem(j + o, ntp)),
                device_id_type=MESH,
            )
            copy.start()
            pending.append(copy)

    def from_tp(buf, ssem, rsem):
        for o in range(1, ntp):
            slot = lax.rem(j + ntp - o, ntp)
            pltpu.make_async_remote_copy(
                src_ref=buf.at[slot],
                dst_ref=buf.at[slot],
                send_sem=ssem.at[o],
                recv_sem=rsem.at[o],
                device_id=(i, slot),
                device_id_type=MESH,
            ).wait_recv()

    l_tok.wait()
    l_g1.wait()
    l_g2.wait()
    gat[j, 0:B, :] = tokens_v[...].astype(F32)
    gat[j, B : B + 1, :] = gain1_v[...].astype(F32)
    gat[j, B + 1 : B + 2, :] = gain2_v[...].astype(F32)
    gat[j, B + 2 : 8, :] = jnp.zeros((6 - B, c0), F32)
    pl.semaphore_wait(barrier, N - 1)
    to_tp(gat, s1, r1)
    l_wq.wait()
    l_wf.wait()
    from_tp(gat, s1, r1)
    for t in range(ntp):
        xbuf[:, t * c0 : (t + 1) * c0] = gat[t]

    every = xbuf[...]
    rows = every[0:B]
    gain_b = jnp.broadcast_to(every[B : B + 1], every.shape)
    row_id = iota(every.shape, 0)
    lhs = jnp.where(row_id < B, every * gain_b, jnp.where(row_id == B, gain_b, 0.0)).astype(BF16)

    def product(weight):
        return jnp.dot(lhs, weight[...], preferred_element_type=F32)

    def spread(buf, at, row, count):
        if count < B:
            buf[i, :, at : at + LANES] = jnp.zeros((B, LANES), F32)
        for r in range(count):
            buf[i, r : r + 1, at : at + LANES] = row[:, r * LANES : (r + 1) * LANES]

    part = product(wq_v)
    qmsg[i, :, 0:C] = part[0:B]
    spread(qmsg, C, part[B : B + 1], nc)
    part = across(lhs, wf_v[...])
    aux = C + LANES
    qmsg[i, :, aux : aux + LANES] = jnp.zeros((B, LANES), F32)
    qmsg[i, :, aux : aux + H] = part[0:B]
    qmsg[i, :, aux + H : aux + 2 * H] = jnp.broadcast_to(part[B : B + 1], (B, H))
    qmsg[i, :, aux + 2 * H : aux + 2 * H + 1] = jnp.sum(rows, axis=1, keepdims=True)
    qmsg[i, :, aux + 2 * H + 1 : aux + 2 * H + 2] = jnp.sum(rows * rows, axis=1, keepdims=True)
    to_kv(qmsg, sq, rq)

    l_wk.wait()
    part = product(wk_v)
    kvmsg[i, :, 0:C] = part[0:B]
    spread(kvmsg, 2 * C, part[B : B + 1], nc)
    l_wv.wait()
    part = product(wv_v)
    kvmsg[i, :, C : 2 * C] = part[0:B]
    spread(kvmsg, 2 * C + LANES, part[B : B + 1], nc)
    spread(kvmsg, 2 * C + 2 * LANES, every[B + 1 : B + 2], nr)
    to_kv(kvmsg, sk, rk)

    l_pf.wait()
    later = (iota((LANES, LANES), 0) > iota((LANES, LANES), 1)).astype(F32)
    carry = jnp.zeros((B * h, 1), F32)
    for c in reversed(range(S // LANES)):
        cols = slice(c * LANES, (c + 1) * LANES)
        chunk = jnp.concatenate([pf_v[b, :, cols] for b in range(B)], axis=0)
        inside = jnp.dot(chunk, later, precision=HIGHEST, preferred_element_type=F32)
        whole = inside + carry
        for b in range(B):
            sfx[b, :, cols] = whole[b * h : (b + 1) * h]
        carry = carry + (inside[:, 0:1] + chunk[:, 0:1])

    from_kv(qmsg, sq, rq)
    total = qmsg[0]
    for n in range(1, nkv):
        total = total + qmsg[n]
    moments = total[:, aux + 2 * H : aux + 2 * H + 2]
    mean, factor = row_scales(moments[:, 0:1], moments[:, 1:2], D)

    def whole_row(array, at, count):
        return jnp.concatenate([array[r : r + 1, at : at + LANES] for r in range(count)], axis=1)

    def finish(product_, gain_row):
        return factor * (product_ - mean * gain_row)

    query = finish(total[:, 0:C], whole_row(total, C, nc)).astype(BF16).astype(F32)

    head_of = iota((h, C), 1) // hd
    mine = head_of == iota((h, C), 0)
    head_row = iota((h, LANES), 0)
    lane = iota((h, LANES), 1)
    for b in range(B):
        spread_q = jnp.where(mine, jnp.broadcast_to(query[b : b + 1], (h, C)), 0.0).astype(BF16)
        l_pk[b].wait()
        logits = across(spread_q, pk_v[b]) * scale + sfx[b]
        top = jnp.max(logits, axis=1, keepdims=True)
        weights = jnp.exp(logits - top)
        amount = jnp.sum(weights, axis=1, keepdims=True)
        l_pv[b].wait()
        mixed = jnp.dot(weights.astype(BF16), pv_v[b], preferred_element_type=F32)
        mixbuf[b : b + 1, :] = jnp.sum(jnp.where(mine, mixed, 0.0), axis=0, keepdims=True)
        marks = (
            jnp.where(lane == head_row, top, 0.0)
            + jnp.where(lane == head_row + 32, amount, 0.0)
            + jnp.where(lane == head_row + 64, carry[b * h : (b + 1) * h], 0.0)
        )
        astat[i, b : b + 1, :] = jnp.sum(marks, axis=0, keepdims=True)
    amix[i] = mixbuf[...].astype(BF16)
    to_kv(astat, st, rt)
    to_kv(amix, sa, ra)

    from_kv(kvmsg, sk, rk)
    pair = kvmsg[0, :, 0 : 2 * C + 2 * LANES]
    for n in range(1, nkv):
        pair = pair + kvmsg[n, :, 0 : 2 * C + 2 * LANES]
    for n in range(nkv):
        for r in range(nr):
            at = n * R + r * LANES
            gbuf[0:1, at : at + LANES] = kvmsg[n, r : r + 1, 2 * C + 2 * LANES : 2 * C + 3 * LANES]
    new_keys = finish(pair[:, 0:C], whole_row(pair, 2 * C, nc)).astype(BF16)
    new_values = finish(pair[:, C : 2 * C], whole_row(pair, 2 * C + LANES, nc)).astype(BF16)
    nk_ref[...] = new_keys
    nv_ref[...] = new_values
    pre = finish(total[:, aux : aux + H], total[:, aux + H : aux + 2 * H])
    pick = (iota((H, LANES), 0) == iota((H, LANES), 1) + j * h).astype(F32)
    l_fb.wait()
    gates = jnp.dot(pre, pick, precision=HIGHEST, preferred_element_type=F32)[:, 0:h] + fb_v[...]
    new_forget = jnp.minimum(gates, 0.0) - jnp.log1p(jnp.exp(-jnp.abs(gates)))
    nf_ref[...] = new_forget
    expand = (iota((LANES, C), 0) == iota((LANES, C), 1) // hd).astype(F32)
    gather = (iota((C, LANES), 0) // hd == iota((C, LANES), 1)).astype(F32)
    own = (
        jnp.dot(
            query * new_keys.astype(F32), gather, precision=HIGHEST, preferred_element_type=F32
        )[:, 0:h]
        * scale
    )
    coef[...] = jnp.zeros(coef.shape, F32)
    l_wo.wait()

    from_kv(astat, st, rt)
    tops, amounts = [None] * nkv, [None] * nkv
    behind = new_forget
    peak = own
    for n in reversed(range(nkv)):
        tops[n] = astat[n, :, 0:h] + behind
        amounts[n] = astat[n, :, 32 : 32 + h]
        behind = behind + astat[n, :, 64 : 64 + h]
        peak = jnp.maximum(peak, tops[n])
    own_part = jnp.exp(own - peak)
    bottom = own_part
    parts = []
    for n in range(nkv):
        parts.append(jnp.exp(tops[n] - peak))
        bottom = bottom + amounts[n] * parts[n]
    for n, one in enumerate(parts + [own_part]):
        coef[n * B : (n + 1) * B, 0:h] = one / bottom
    wide = jnp.dot(coef[...], expand, precision=HIGHEST, preferred_element_type=F32)
    attended = wide[nkv * B : (nkv + 1) * B] * new_values.astype(F32)
    from_kv(amix, sa, ra)
    for n in range(nkv):
        attended = attended + wide[n * B : (n + 1) * B] * amix[n].astype(F32)

    bmsg[j] = jnp.dot(attended.astype(BF16), wo_v[...], preferred_element_type=F32)
    to_tp(bmsg, sb, rb)
    from_tp(bmsg, sb, rb)
    branch = bmsg[0]
    for t in range(1, ntp):
        branch = branch + bmsg[t]
    middle = (rows + branch).astype(BF16)
    mmsg[i] = middle
    to_kv(mmsg, sm, rm)
    for t in range(ntp):
        mpieces[t] = middle[:, t * c0 : (t + 1) * c0].astype(F32)
    l_wg.wait()
    l_wu.wait()
    l_wd.wait()
    from_kv(mmsg, sm, rm)
    for n in range(nkv):
        mbuf[:, n * R : (n + 1) * R] = mmsg[n].astype(F32)
    wide_mid = mbuf[...]
    mid_mean, mid_scale = row_scales(
        jnp.sum(wide_mid, axis=1, keepdims=True),
        jnp.sum(wide_mid * wide_mid, axis=1, keepdims=True),
        D,
    )
    normed = ((wide_mid - mid_mean) * mid_scale * gbuf[...]).astype(BF16)
    gate = across(normed, wg_v[...])
    up = across(normed, wu_v[...])
    hidden = (gate / (1.0 + jnp.exp(-gate)) * up).astype(BF16)
    down = jnp.dot(hidden, wd_v[...], preferred_element_type=F32)
    for p in range(N):
        fsend[p] = down[:, p * c0 : (p + 1) * c0]
    me = i * ntp + j
    for a in reversed(range(nkv)):
        for b in range(ntp):
            if a or b:
                there = (lax.rem(i + a, nkv), lax.rem(j + b, ntp))
                copy = pltpu.make_async_remote_copy(
                    src_ref=fsend.at[there[0] * ntp + there[1]],
                    dst_ref=frecv.at[me],
                    send_sem=sf.at[a * ntp + b],
                    recv_sem=rf.at[a * ntp + b],
                    device_id=there,
                    device_id_type=MESH,
                )
                copy.start()
                pending.append(copy)
    frecv[me] = fsend[me]
    for a in range(nkv):
        for b in range(ntp):
            if a or b:
                there = (lax.rem(i + nkv - a, nkv), lax.rem(j + ntp - b, ntp))
                slot = there[0] * ntp + there[1]
                pltpu.make_async_remote_copy(
                    src_ref=fsend.at[slot],
                    dst_ref=frecv.at[slot],
                    send_sem=sf.at[a * ntp + b],
                    recv_sem=rf.at[a * ntp + b],
                    device_id=there,
                    device_id_type=MESH,
                ).wait_recv()
    channel = frecv[0]
    for p in range(1, N):
        channel = channel + frecv[p]
    out_ref[...] = (mpieces[j] + channel).astype(BF16)
    for copy in pending:
        copy.wait_send()


def hand_over(*refs):
    count = len(refs) // 3
    copies = [
        pltpu.make_async_copy(refs[n], refs[count + n], refs[2 * count + n]) for n in range(count)
    ]
    for copy in copies:
        copy.start()
    for copy in copies:
        copy.wait()


def local(nkv, ntp, *arrays):
    (tokens, gain1, wq, wk, wv, wf, fb, pk, pv, pf, wo, gain2, wg, wu, wd) = arrays
    gain1, gain2, fb = gain1[None, :], gain2[None, :], fb[None, :]
    wf, wg, wu = wf.T, wg.T, wu.T
    arrays = (tokens, gain1, wq, wk, wv, wf, fb, pk, pv, pf, wo, gain2, wg, wu, wd)
    B, c0 = tokens.shape
    R, C = wq.shape
    h = fb.shape[1]
    F, D = wg.shape
    S = pk.shape[1]
    N = nkv * ntp
    dma = lambda n: pltpu.SemaphoreType.DMA((n,))
    scratch = [
        pltpu.VMEM(a.shape, a.dtype)
        for a in (tokens, gain1, gain2, wq, wk, wv, wf, fb, pk, pv, pf, wo, wg, wu, wd)
    ]
    scratch += [
        pltpu.VMEM((ntp, 8, c0), F32),
        pltpu.VMEM((8, R), F32),
        pltpu.VMEM((nkv, B, C + 2 * LANES), F32),
        pltpu.VMEM((nkv, B, 2 * C + 3 * LANES), F32),
        pltpu.VMEM((B, h, S), F32),
        pltpu.VMEM((B, C), F32),
        pltpu.VMEM((nkv, B, C), BF16),
        pltpu.VMEM((nkv, B, LANES), F32),
        pltpu.VMEM(((nkv + 1) * B, LANES), F32),
        pltpu.VMEM((ntp, B, R), F32),
        pltpu.VMEM((ntp, B, c0), F32),
        pltpu.VMEM((nkv, B, R), BF16),
        pltpu.VMEM((B, D), F32),
        pltpu.VMEM((1, D), F32),
        pltpu.VMEM((N, B, c0), F32),
        pltpu.VMEM((N, B, c0), F32),
        dma(13 + 2 * B),
    ]
    for n in (ntp, nkv, nkv, nkv, nkv, ntp, nkv, N):
        scratch += [dma(n), dma(n)]
    vmem = pl.BlockSpec(memory_space=pltpu.VMEM)
    results = pl.pallas_call(
        functools.partial(kernel, nkv, ntp),
        out_shape=(
            jax.ShapeDtypeStruct((B, c0), BF16),
            jax.ShapeDtypeStruct((B, C), BF16),
            jax.ShapeDtypeStruct((B, C), BF16),
            jax.ShapeDtypeStruct((B, h), F32),
        ),
        in_specs=[pl.BlockSpec(memory_space=pl.ANY)] * len(arrays),
        out_specs=(vmem,) * 4,
        scratch_shapes=scratch,
        compiler_params=pltpu.CompilerParams(
            collective_id=0, has_side_effects=True, vmem_limit_bytes=60 * 2**20
        ),
    )(*arrays)
    return pl.pallas_call(
        hand_over,
        out_shape=tuple(jax.ShapeDtypeStruct(one.shape, one.dtype) for one in results),
        in_specs=[vmem] * 4,
        out_specs=(pl.BlockSpec(memory_space=pl.ANY),) * 4,
        scratch_shapes=[pltpu.SemaphoreType.DMA] * 4,
    )(*results)


def solution(mesh):
    in_specs = (
        P(None, ("kv", "tp")),
        P(("kv", "tp")),
        P("kv", "tp"),
        P("kv", "tp"),
        P("kv", "tp"),
        P("kv", None),
        P("tp"),
        P(None, "kv", "tp"),
        P(None, "kv", "tp"),
        P(None, "tp", "kv"),
        P("tp", "kv"),
        P(("kv", "tp")),
        P(None, ("kv", "tp")),
        P(None, ("kv", "tp")),
        P(("kv", "tp"), None),
    )
    out_specs = (P(None, ("kv", "tp")), P(None, "tp"), P(None, "tp"), P(None, "tp"))
    step = functools.partial(local, mesh.shape["kv"], mesh.shape["tp"])
    return jax.shard_map(step, mesh=mesh, in_specs=in_specs, out_specs=out_specs, check_vma=False)
```

```python
import functools

import jax
import jax.numpy as jnp
from jax import lax
from jax.experimental import pallas as pl
from jax.experimental.pallas import tpu as pltpu
from jax.sharding import PartitionSpec as P

epsilon = 1e-05
MESH = pl.DeviceIdType.MESH
HIGHEST = lax.Precision.HIGHEST
LANES = 128
F32 = jnp.float32
BF16 = jnp.bfloat16


def iota(shape, dim):
    return lax.broadcasted_iota(jnp.int32, shape, dim)


def across(left, right):
    return lax.dot_general(left, right, (((1,), (1,)), ((), ())), preferred_element_type=F32)


def row_scales(first_sum, second_sum, row_width):
    row_mean = first_sum / row_width
    spread = jnp.maximum(second_sum / row_width - row_mean * row_mean, 0.0) + epsilon
    return (row_mean, lax.rsqrt(spread))


def kernel(
    nkv,
    ntp,
    tokens_h,
    gain1_h,
    wq_h,
    wk_h,
    wv_h,
    wf_h,
    fb_h,
    pk_h,
    pv_h,
    pf_h,
    wo_h,
    gain2_h,
    wg_h,
    wu_h,
    wd_h,
    out_ref,
    nk_ref,
    nv_ref,
    nf_ref,
    tokens_v,
    gain1_v,
    gain2_v,
    wq_v,
    wk_v,
    wv_v,
    wf_v,
    fb_v,
    pk_v,
    pv_v,
    pf_v,
    wo_v,
    wg_v,
    wu_v,
    wd_v,
    gat,
    xbuf,
    qmsg,
    kvmsg,
    sfx,
    mixbuf,
    amix,
    astat,
    coef,
    bmsg,
    mpieces,
    mmsg,
    mbuf,
    gbuf,
    fsend,
    frecv,
    in_sem,
    s1,
    r1,
    sq,
    rq,
    sk,
    rk,
    sa,
    ra,
    st,
    rt,
    sb,
    rb,
    sm,
    rm,
    sf,
    rf,
):
    i = lax.axis_index("kv")
    j = lax.axis_index("tp")
    B, c0 = tokens_v.shape
    R, C = wq_v.shape
    H = wf_v.shape[0]
    h = fb_v.shape[1]
    hd = C // h
    S = pk_v.shape[1]
    F, D = wg_v.shape
    N = nkv * ntp
    scale = hd ** (-0.5)
    nc, nr = C // LANES, R // LANES

    plan = [
        (tokens_h, tokens_v),
        (gain1_h, gain1_v),
        (gain2_h, gain2_v),
        (wq_h, wq_v),
        (wf_h, wf_v),
        (wk_h, wk_v),
        (wv_h, wv_v),
        (pf_h, pf_v),
    ]
    plan += [(pk_h.at[b], pk_v.at[b]) for b in range(B)]
    plan += [(pv_h.at[b], pv_v.at[b]) for b in range(B)]
    plan += [(fb_h, fb_v), (wo_h, wo_v), (wg_h, wg_v), (wu_h, wu_v), (wd_h, wd_v)]
    loads = [
        pltpu.make_async_copy(src, dst, in_sem.at[n]) for n, (src, dst) in enumerate(plan)
    ]
    for load in loads:
        load.start()
    l_tok, l_g1, l_g2, l_wq, l_wf, l_wk, l_wv, l_pf = loads[:8]
    l_pk, l_pv = loads[8 : 8 + B], loads[8 + B : 8 + 2 * B]
    l_fb, l_wo, l_wg, l_wu, l_wd = loads[8 + 2 * B :]

    barrier = pltpu.get_barrier_semaphore()
    for a in range(nkv):
        for b in range(ntp):
            if a or b:
                pl.semaphore_signal(
                    barrier,
                    inc=1,
                    device_id=(lax.rem(i + a, nkv), lax.rem(j + b, ntp)),
                    device_id_type=MESH,
                )

    pending = []

    def to_kv(buf, ssem, rsem):
        for o in range(1, nkv):
            copy = pltpu.make_async_remote_copy(
                src_ref=buf.at[i],
                dst_ref=buf.at[i],
                send_sem=ssem.at[o],
                recv_sem=rsem.at[o],
                device_id=(lax.rem(i + o, nkv), j),
                device_id_type=MESH,
            )
            copy.start()
            pending.append(copy)

    def from_kv(buf, ssem, rsem):
        for o in range(1, nkv):
            slot = lax.rem(i + nkv - o, nkv)
            pltpu.make_async_remote_copy(
                src_ref=buf.at[slot],
                dst_ref=buf.at[slot],
                send_sem=ssem.at[o],
                recv_sem=rsem.at[o],
                device_id=(slot, j),
                device_id_type=MESH,
            ).wait_recv()

    def to_tp(buf, ssem, rsem):
        for o in range(1, ntp):
            copy = pltpu.make_async_remote_copy(
                src_ref=buf.at[j],
                dst_ref=buf.at[j],
                send_sem=ssem.at[o],
                recv_sem=rsem.at[o],
                device_id=(i, lax.rem(j + o, ntp)),
                device_id_type=MESH,
            )
            copy.start()
            pending.append(copy)

    def from_tp(buf, ssem, rsem):
        for o in range(1, ntp):
            slot = lax.rem(j + ntp - o, ntp)
            pltpu.make_async_remote_copy(
                src_ref=buf.at[slot],
                dst_ref=buf.at[slot],
                send_sem=ssem.at[o],
                recv_sem=rsem.at[o],
                device_id=(i, slot),
                device_id_type=MESH,
            ).wait_recv()

    l_tok.wait()
    l_g1.wait()
    l_g2.wait()
    gat[j, 0:B, :] = tokens_v[...].astype(F32)
    gat[j, B : B + 1, :] = gain1_v[...].astype(F32)
    gat[j, B + 1 : B + 2, :] = gain2_v[...].astype(F32)
    gat[j, B + 2 : 8, :] = jnp.zeros((6 - B, c0), F32)
    pl.semaphore_wait(barrier, N - 1)
    to_tp(gat, s1, r1)
    l_wq.wait()
    l_wf.wait()
    from_tp(gat, s1, r1)
    for t in range(ntp):
        xbuf[:, t * c0 : (t + 1) * c0] = gat[t]

    every = xbuf[...]
    rows = every[0:B]
    gain_b = jnp.broadcast_to(every[B : B + 1], every.shape)
    row_id = iota(every.shape, 0)
    lhs = jnp.where(row_id < B, every * gain_b, jnp.where(row_id == B, gain_b, 0.0)).astype(BF16)

    def product(weight):
        return jnp.dot(lhs, weight[...], preferred_element_type=F32)

    def spread(buf, at, row, count):
        if count < B:
            buf[i, :, at : at + LANES] = jnp.zeros((B, LANES), F32)
        for r in range(count):
            buf[i, r : r + 1, at : at + LANES] = row[:, r * LANES : (r + 1) * LANES]

    part = product(wq_v)
    qmsg[i, :, 0:C] = part[0:B]
    spread(qmsg, C, part[B : B + 1], nc)
    part = across(lhs, wf_v[...])
    aux = C + LANES
    qmsg[i, :, aux : aux + LANES] = jnp.zeros((B, LANES), F32)
    qmsg[i, :, aux : aux + H] = part[0:B]
    qmsg[i, :, aux + H : aux + 2 * H] = jnp.broadcast_to(part[B : B + 1], (B, H))
    qmsg[i, :, aux + 2 * H : aux + 2 * H + 1] = jnp.sum(rows, axis=1, keepdims=True)
    qmsg[i, :, aux + 2 * H + 1 : aux + 2 * H + 2] = jnp.sum(rows * rows, axis=1, keepdims=True)
    to_kv(qmsg, sq, rq)

    l_wk.wait()
    part = product(wk_v)
    kvmsg[i, :, 0:C] = part[0:B]
    spread(kvmsg, 2 * C, part[B : B + 1], nc)
    l_wv.wait()
    part = product(wv_v)
    kvmsg[i, :, C : 2 * C] = part[0:B]
    spread(kvmsg, 2 * C + LANES, part[B : B + 1], nc)
    spread(kvmsg, 2 * C + 2 * LANES, every[B + 1 : B + 2], nr)
    to_kv(kvmsg, sk, rk)

    l_pf.wait()
    later = (iota((LANES, LANES), 0) > iota((LANES, LANES), 1)).astype(F32)
    carry = jnp.zeros((B * h, 1), F32)
    for c in reversed(range(S // LANES)):
        cols = slice(c * LANES, (c + 1) * LANES)
        chunk = jnp.concatenate([pf_v[b, :, cols] for b in range(B)], axis=0)
        inside = jnp.dot(chunk, later, precision=HIGHEST, preferred_element_type=F32)
        whole = inside + carry
        for b in range(B):
            sfx[b, :, cols] = whole[b * h : (b + 1) * h]
        carry = carry + (inside[:, 0:1] + chunk[:, 0:1])

    for load in l_pk + l_pv + [l_fb, l_wo, l_wg, l_wu, l_wd]:
        load.wait()

    from_kv(qmsg, sq, rq)
    total = qmsg[0]
    for n in range(1, nkv):
        total = total + qmsg[n]
    moments = total[:, aux + 2 * H : aux + 2 * H + 2]
    mean, factor = row_scales(moments[:, 0:1], moments[:, 1:2], D)

    def whole_row(array, at, count):
        return jnp.concatenate([array[r : r + 1, at : at + LANES] for r in range(count)], axis=1)

    def finish(product_, gain_row):
        return factor * (product_ - mean * gain_row)

    query = finish(total[:, 0:C], whole_row(total, C, nc)).astype(BF16).astype(F32)

    head_of = iota((h, C), 1) // hd
    mine = head_of == iota((h, C), 0)
    head_row = iota((h, LANES), 0)
    lane = iota((h, LANES), 1)
    for b in range(B):
        spread_q = jnp.where(mine, jnp.broadcast_to(query[b : b + 1], (h, C)), 0.0).astype(BF16)
        logits = across(spread_q, pk_v[b]) * scale + sfx[b]
        top = jnp.max(logits, axis=1, keepdims=True)
        weights = jnp.exp(logits - top)
        amount = jnp.sum(weights, axis=1, keepdims=True)
        mixed = jnp.dot(weights.astype(BF16), pv_v[b], preferred_element_type=F32)
        mixbuf[b : b + 1, :] = jnp.sum(jnp.where(mine, mixed, 0.0), axis=0, keepdims=True)
        marks = (
            jnp.where(lane == head_row, top, 0.0)
            + jnp.where(lane == head_row + 32, amount, 0.0)
            + jnp.where(lane == head_row + 64, carry[b * h : (b + 1) * h], 0.0)
        )
        astat[i, b : b + 1, :] = jnp.sum(marks, axis=0, keepdims=True)
    amix[i] = mixbuf[...].astype(BF16)
    to_kv(astat, st, rt)
    to_kv(amix, sa, ra)

    from_kv(kvmsg, sk, rk)
    pair = kvmsg[0, :, 0 : 2 * C + 2 * LANES]
    for n in range(1, nkv):
        pair = pair + kvmsg[n, :, 0 : 2 * C + 2 * LANES]
    for n in range(nkv):
        for r in range(nr):
            at = n * R + r * LANES
            gbuf[0:1, at : at + LANES] = kvmsg[n, r : r + 1, 2 * C + 2 * LANES : 2 * C + 3 * LANES]
    new_keys = finish(pair[:, 0:C], whole_row(pair, 2 * C, nc)).astype(BF16)
    new_values = finish(pair[:, C : 2 * C], whole_row(pair, 2 * C + LANES, nc)).astype(BF16)
    nk_ref[...] = new_keys
    nv_ref[...] = new_values
    pre = finish(total[:, aux : aux + H], total[:, aux + H : aux + 2 * H])
    pick = (iota((H, LANES), 0) == iota((H, LANES), 1) + j * h).astype(F32)
    gates = jnp.dot(pre, pick, precision=HIGHEST, preferred_element_type=F32)[:, 0:h] + fb_v[...]
    new_forget = jnp.minimum(gates, 0.0) - jnp.log1p(jnp.exp(-jnp.abs(gates)))
    nf_ref[...] = new_forget
    expand = (iota((LANES, C), 0) == iota((LANES, C), 1) // hd).astype(F32)
    gather = (iota((C, LANES), 0) // hd == iota((C, LANES), 1)).astype(F32)
    own = (
        jnp.dot(
            query * new_keys.astype(F32), gather, precision=HIGHEST, preferred_element_type=F32
        )[:, 0:h]
        * scale
    )
    coef[...] = jnp.zeros(coef.shape, F32)

    from_kv(astat, st, rt)
    tops, amounts = [None] * nkv, [None] * nkv
    behind = new_forget
    peak = own
    for n in reversed(range(nkv)):
        tops[n] = astat[n, :, 0:h] + behind
        amounts[n] = astat[n, :, 32 : 32 + h]
        behind = behind + astat[n, :, 64 : 64 + h]
        peak = jnp.maximum(peak, tops[n])
    own_part = jnp.exp(own - peak)
    bottom = own_part
    parts = []
    for n in range(nkv):
        parts.append(jnp.exp(tops[n] - peak))
        bottom = bottom + amounts[n] * parts[n]
    for n, one in enumerate(parts + [own_part]):
        coef[n * B : (n + 1) * B, 0:h] = one / bottom
    wide = jnp.dot(coef[...], expand, precision=HIGHEST, preferred_element_type=F32)
    attended = wide[nkv * B : (nkv + 1) * B] * new_values.astype(F32)
    from_kv(amix, sa, ra)
    for n in range(nkv):
        attended = attended + wide[n * B : (n + 1) * B] * amix[n].astype(F32)

    bmsg[j] = jnp.dot(attended.astype(BF16), wo_v[...], preferred_element_type=F32)
    to_tp(bmsg, sb, rb)
    from_tp(bmsg, sb, rb)
    branch = bmsg[0]
    for t in range(1, ntp):
        branch = branch + bmsg[t]
    middle = (rows + branch).astype(BF16)
    mmsg[i] = middle
    to_kv(mmsg, sm, rm)
    for t in range(ntp):
        mpieces[t] = middle[:, t * c0 : (t + 1) * c0].astype(F32)
    from_kv(mmsg, sm, rm)
    for n in range(nkv):
        mbuf[:, n * R : (n + 1) * R] = mmsg[n].astype(F32)
    wide_mid = mbuf[...]
    mid_mean, mid_scale = row_scales(
        jnp.sum(wide_mid, axis=1, keepdims=True),
        jnp.sum(wide_mid * wide_mid, axis=1, keepdims=True),
        D,
    )
    normed = ((wide_mid - mid_mean) * mid_scale * gbuf[...]).astype(BF16)
    gate = across(normed, wg_v[...])
    up = across(normed, wu_v[...])
    hidden = (gate / (1.0 + jnp.exp(-gate)) * up).astype(BF16)
    down = jnp.dot(hidden, wd_v[...], preferred_element_type=F32)
    for p in range(N):
        fsend[p] = down[:, p * c0 : (p + 1) * c0]
    me = i * ntp + j
    for a in reversed(range(nkv)):
        for b in range(ntp):
            if a or b:
                there = (lax.rem(i + a, nkv), lax.rem(j + b, ntp))
                copy = pltpu.make_async_remote_copy(
                    src_ref=fsend.at[there[0] * ntp + there[1]],
                    dst_ref=frecv.at[me],
                    send_sem=sf.at[a * ntp + b],
                    recv_sem=rf.at[a * ntp + b],
                    device_id=there,
                    device_id_type=MESH,
                )
                copy.start()
                pending.append(copy)
    frecv[me] = fsend[me]
    for a in range(nkv):
        for b in range(ntp):
            if a or b:
                there = (lax.rem(i + nkv - a, nkv), lax.rem(j + ntp - b, ntp))
                slot = there[0] * ntp + there[1]
                pltpu.make_async_remote_copy(
                    src_ref=fsend.at[slot],
                    dst_ref=frecv.at[slot],
                    send_sem=sf.at[a * ntp + b],
                    recv_sem=rf.at[a * ntp + b],
                    device_id=there,
                    device_id_type=MESH,
                ).wait_recv()
    channel = frecv[0]
    for p in range(1, N):
        channel = channel + frecv[p]
    out_ref[...] = (mpieces[j] + channel).astype(BF16)
    for copy in pending:
        copy.wait_send()


def hand_over(*refs):
    count = len(refs) // 3
    copies = [
        pltpu.make_async_copy(refs[n], refs[count + n], refs[2 * count + n]) for n in range(count)
    ]
    for copy in copies:
        copy.start()
    for copy in copies:
        copy.wait()


def local(nkv, ntp, *arrays):
    (tokens, gain1, wq, wk, wv, wf, fb, pk, pv, pf, wo, gain2, wg, wu, wd) = arrays
    gain1, gain2, fb = gain1[None, :], gain2[None, :], fb[None, :]
    wf, wg, wu = wf.T, wg.T, wu.T
    arrays = (tokens, gain1, wq, wk, wv, wf, fb, pk, pv, pf, wo, gain2, wg, wu, wd)
    B, c0 = tokens.shape
    R, C = wq.shape
    h = fb.shape[1]
    F, D = wg.shape
    S = pk.shape[1]
    N = nkv * ntp
    dma = lambda n: pltpu.SemaphoreType.DMA((n,))
    scratch = [
        pltpu.VMEM(a.shape, a.dtype)
        for a in (tokens, gain1, gain2, wq, wk, wv, wf, fb, pk, pv, pf, wo, wg, wu, wd)
    ]
    scratch += [
        pltpu.VMEM((ntp, 8, c0), F32),
        pltpu.VMEM((8, R), F32),
        pltpu.VMEM((nkv, B, C + 2 * LANES), F32),
        pltpu.VMEM((nkv, B, 2 * C + 3 * LANES), F32),
        pltpu.VMEM((B, h, S), F32),
        pltpu.VMEM((B, C), F32),
        pltpu.VMEM((nkv, B, C), BF16),
        pltpu.VMEM((nkv, B, LANES), F32),
        pltpu.VMEM(((nkv + 1) * B, LANES), F32),
        pltpu.VMEM((ntp, B, R), F32),
        pltpu.VMEM((ntp, B, c0), F32),
        pltpu.VMEM((nkv, B, R), BF16),
        pltpu.VMEM((B, D), F32),
        pltpu.VMEM((1, D), F32),
        pltpu.VMEM((N, B, c0), F32),
        pltpu.VMEM((N, B, c0), F32),
        dma(13 + 2 * B),
    ]
    for n in (ntp, nkv, nkv, nkv, nkv, ntp, nkv, N):
        scratch += [dma(n), dma(n)]
    vmem = pl.BlockSpec(memory_space=pltpu.VMEM)
    results = pl.pallas_call(
        functools.partial(kernel, nkv, ntp),
        out_shape=(
            jax.ShapeDtypeStruct((B, c0), BF16),
            jax.ShapeDtypeStruct((B, C), BF16),
            jax.ShapeDtypeStruct((B, C), BF16),
            jax.ShapeDtypeStruct((B, h), F32),
        ),
        in_specs=[pl.BlockSpec(memory_space=pl.ANY)] * len(arrays),
        out_specs=(vmem,) * 4,
        scratch_shapes=scratch,
        compiler_params=pltpu.CompilerParams(
            collective_id=0, has_side_effects=True, vmem_limit_bytes=60 * 2**20
        ),
    )(*arrays)
    return pl.pallas_call(
        hand_over,
        out_shape=tuple(jax.ShapeDtypeStruct(one.shape, one.dtype) for one in results),
        in_specs=[vmem] * 4,
        out_specs=(pl.BlockSpec(memory_space=pl.ANY),) * 4,
        scratch_shapes=[pltpu.SemaphoreType.DMA] * 4,
    )(*results)


def solution(mesh):
    in_specs = (
        P(None, ("kv", "tp")),
        P(("kv", "tp")),
        P("kv", "tp"),
        P("kv", "tp"),
        P("kv", "tp"),
        P("kv", None),
        P("tp"),
        P(None, "kv", "tp"),
        P(None, "kv", "tp"),
        P(None, "tp", "kv"),
        P("tp", "kv"),
        P(("kv", "tp")),
        P(None, ("kv", "tp")),
        P(None, ("kv", "tp")),
        P(("kv", "tp"), None),
    )
    out_specs = (P(None, ("kv", "tp")), P(None, "tp"), P(None, "tp"), P(None, "tp"))
    step = functools.partial(local, mesh.shape["kv"], mesh.shape["tp"])
    return jax.shard_map(step, mesh=mesh, in_specs=in_specs, out_specs=out_specs, check_vma=False)
```
